256 devices in a mesh: grp: 2 (over y), sp: 32 (over z, core), tp: 4 (over x).
Axes of the slice: x: 4, y: 2, z: 16, core: 2. Of those that a mesh axis runs over, the one named last changes fastest.
The devices are a block of a 4x16x16 slice.
Arguments:
- resid: bfloat16 [32768, 2048], P(('grp', 'sp', 'tp')), parts along dimension 0, may hold values from -6 to 6
- pool_input: bfloat16 [32768, 512], P(('grp', 'sp'), 'tp'), parts along dimension 0, may hold values from -6 to 6
- group_map: bfloat16 [4, 128, 128], P('tp'), may hold values from -0.5 to 0.5
- pool_scale: bfloat16 [512], P('tp'), may hold values from 0.099609375 to 1.8984375
- out_proj: bfloat16 [512, 2048], P('tp'), may hold values from -0.25 to 0.25
- norm_gain: bfloat16 [2048], replicated, may hold values from 0.099609375 to 1.8984375
- routes: int32 [32768, 2], P(('grp', 'sp', 'tp')), parts along dimension 0, may hold values from 0 to 31, all different within a row; in each aligned block of 128 rows (0 to 127, 128 to 255, ...) at most 10 rows name the same one
- route_weight: float32 [32768, 2], P(('grp', 'sp', 'tp')), parts along dimension 0, may hold values from 0.2 to 1
- expert_gate: bfloat16 [32, 2048, 3584], P('sp', None, 'tp'), may hold values from -0.125 to 0.125
- expert_up: bfloat16 [32, 2048, 3584], P('sp', None, 'tp'), may hold values from -0.125 to 0.125
- expert_down: bfloat16 [32, 3584, 2048], P('sp', 'tp'), may hold values from -0.09375 to 0.09375
Outputs:
- layer_out: bfloat16 [32768, 2048], P(('grp', 'sp', 'tp')), parts along dimension 0
The draws below stay inside these ranges and needn't reach their ends.
There are 2 independent parts, one for each index of `grp`. The reference program is written for one: setup_inputs(seed, part) draws one part's arguments, and reference() takes and returns one part's arrays. A program takes and returns all parts, laid end to end along the dimension named above; an argument that names none is the same for every part. Nothing has to cross between parts.
Inputs may be any that keep to these rules, and one draw needn't show every extreme that they name: The 2 routes of a token differ. Among the tokens of one device (aligned blocks of 128 tokens), no expert is named more than 10 times, and in every draw some device names some expert exactly 10 times.
All inputs are finite; a program needn't handle non-finite values.
Results may differ from the reference program's by a relative error of at most 0.011.
Values may be sent and summed in bfloat16 or wider, within the bound.
A program may use at most 128 MiB of HBM per device.

```python
import math
import jax
import jax.numpy as jnp
import numpy as np
from jax import lax

D = 2048
GROUPS = 4
POOL_WIDTH = 512
GROUP_DIM = 128
EXPERT_FF = 3584
TOPK = 2
EXPERTS = 32
ROWS_DEV = 128
TOKENS = 16384
CAP = 10
N_SP = 32
N_TP = 4


def levels(key, dims, split, low, top_value):
    loudness = 1.0
    for position, blocks in split:
        steps = jax.random.uniform(jax.random.fold_in(jax.random.fold_in(key, 6), position), (blocks,), jnp.float32, low / len(split), top_value / len(split))
        loudness = loudness * jnp.repeat(jnp.exp(steps), dims[position] // blocks).reshape((-1,) + (1,) * (len(dims) - 1 - position))
    return loudness


def deal_out(own_key, own, number, rows, count, top, most, lean):
    sequence = jax.random.permutation(own_key, count)
    crowded, common = portions_of(count, rows * top, most, lean, True), portions_of(count, rows * top, most, lean, False)
    places = jnp.arange(count)

    def named(sizes, rotation):
        used = int((sizes > 0).sum())
        fixed = max(1, used // 4)
        shifted = fixed + (places - fixed + rotation * (used - fixed)) % max(1, count - fixed)
        return jnp.zeros((count,), jnp.int32).at[sequence[jnp.where(places < fixed, places, shifted)]].set(jnp.asarray(sizes, jnp.int32))

    sizes = jnp.where(number % 4 == 0, named(crowded, number // 4), named(common, number - number // 4 - 1))
    mixed = jax.random.permutation(jax.random.fold_in(own, 3), count)
    source_of, taker = mixed[0:count // 2 * 2:2], mixed[1:count // 2 * 2:2]
    slack = jnp.minimum(sizes[source_of] - 1, most - sizes[taker]) // 2
    slack = jnp.where((source_of == sequence[0]) | (taker == sequence[0]) | (sizes[taker] == 0), 0, jnp.maximum(slack, 0))
    shifted = jax.random.randint(jax.random.fold_in(own, 4), (count // 2,), 0, 1 << 20) % (slack + 1)
    sizes = sizes.at[source_of].add(-shifted).at[taker].add(shifted)
    members = jnp.searchsorted(jnp.cumsum(sizes), jnp.arange(rows * top), side="right").astype(jnp.int32)
    grid = members.reshape(top, rows).T
    grid = grid[jax.random.permutation(jax.random.fold_in(own, 1), rows)]
    rotation = jax.random.randint(jax.random.fold_in(own, 2), (rows, 1), 0, top)
    return jnp.take_along_axis(grid, (jnp.arange(top)[None, :] + rotation) % top, axis=1)


def portions_of(amount, total, reach, lean, full):
    portions = [(1 << 20) // math.isqrt(grade ** lean) + 1 for grade in range(1, amount + 1)]
    largest = reach if full else min(reach, max(-(-total // amount), total * portions[0] // sum(portions)))
    least = 1 if total - largest >= amount - 1 else 0
    counts, rest = [largest] + [least] * (amount - 1), total - largest - least * (amount - 1)
    while rest > 0:
        candidates = [i for i in range(1, amount) if counts[i] < largest] or [i for i in range(1, amount) if counts[i] < reach]
        mass, remaining = sum([portions[i] for i in candidates]), rest
        for i in candidates:
            more = min(reach - counts[i], max(1, remaining * portions[i] // mass), rest)
            counts[i] = counts[i] + more
            rest = rest - more
    return np.array(counts)


def bell_draw(key, shape, spread, limit, cuts=(), kind=jnp.bfloat16):
    result = spread * jax.random.normal(key, shape, jnp.float32)
    if cuts:
        result = result * levels(key, shape, cuts, -0.22, 0.18)
    return jnp.clip(result, -limit, limit).astype(kind)


def setup_inputs(seed: int = 0, part: int = 0) -> dict:
    keys = jax.random.split(jax.random.key(seed), 12)
    part_splits = jax.random.split(jax.random.fold_in(keys[11], part), 12)
    resid = bell_draw(part_splits[0], (TOKENS, D), 1.0, 6.0, ((0, 128),))
    pool_input = bell_draw(part_splits[1], (TOKENS, POOL_WIDTH), 1.0, 6.0, ((0, 32), (1, 4)))
    group_map = bell_draw(keys[2], (GROUPS, GROUP_DIM, GROUP_DIM), GROUP_DIM ** -0.5, 0.5, ((0, 4),))
    pool_scale = jnp.clip(1.0 + 0.18 * jax.random.normal(keys[3], (POOL_WIDTH,), jnp.float32), 0.099609375, 1.8984375).astype(jnp.bfloat16)
    out_proj = bell_draw(keys[4], (POOL_WIDTH, D), POOL_WIDTH ** -0.5, 0.25, ((0, 4),))
    norm_gain = jnp.clip(1.0 + 0.18 * jax.random.normal(keys[5], (D,), jnp.float32), 0.099609375, 1.8984375).astype(jnp.bfloat16)
    routes_keys = jax.random.split(jax.random.fold_in(part_splits[6], 1), TOKENS // ROWS_DEV)
    routes_turns = jax.random.permutation(jax.random.fold_in(part_splits[6], 3), TOKENS // ROWS_DEV)
    routes = jax.vmap(lambda own, number: deal_out(jax.random.fold_in(part_splits[6], 2), own, number, ROWS_DEV, EXPERTS, TOPK, CAP, 1))(routes_keys, routes_turns).reshape((TOKENS, TOPK))
    route_weight = jnp.clip(0.2 + 0.8 * jax.random.uniform(part_splits[7], (TOKENS, TOPK), jnp.float32) ** levels(part_splits[7], (TOKENS, TOPK), ((0, 128),), -0.2, 0.2), 0.2, 1.0)
    expert_gate = bell_draw(keys[8], (EXPERTS, D, EXPERT_FF), D ** -0.5, 0.125, ((0, 32), (2, 4)))
    expert_up = bell_draw(keys[9], (EXPERTS, D, EXPERT_FF), D ** -0.5, 0.125, ((0, 32), (2, 4)))
    expert_down = bell_draw(keys[10], (EXPERTS, EXPERT_FF, D), EXPERT_FF ** -0.5, 0.09375, ((0, 32), (1, 4)))
    return {"resid": resid, "pool_input": pool_input, "group_map": group_map, "pool_scale": pool_scale, "out_proj": out_proj, "norm_gain": norm_gain, "routes": routes, "route_weight": route_weight, "expert_gate": expert_gate, "expert_up": expert_up, "expert_down": expert_down}


norm_eps = 1e-06

def pool_group(values, window):
    window_sum = values
    for back in range(1, window):
        window_sum = window_sum + jnp.pad(values[:-back], ((back, 0), (0, 0)))
    divisor = jnp.minimum(jnp.arange(1, values.shape[0] + 1, dtype=jnp.float32), jnp.float32(window))
    return (window_sum / divisor[:, None] - values).astype(jnp.bfloat16)

def reference(resid, pool_input, group_map, pool_scale, out_proj, norm_gain, routes, route_weight, expert_gate, expert_up, expert_down):
    values = pool_input.astype(jnp.float32)
    pieces = []
    for group in range(GROUPS):
        low = group * GROUP_DIM
        pooled = pool_group(values[:, low:low + GROUP_DIM], 2 ** (group + 1))
        product = jnp.dot(pooled, group_map[group], preferred_element_type=jnp.float32)
        pieces.append((product * pool_scale[low:low + GROUP_DIM].astype(jnp.float32)).astype(jnp.bfloat16))
    group_out = jnp.concatenate(pieces, axis=1)
    mix = jnp.dot(group_out, out_proj, preferred_element_type=jnp.float32)
    mixed = (resid.astype(jnp.float32) + mix).astype(jnp.bfloat16)
    residual = mixed.astype(jnp.float32)
    scaled = residual * lax.rsqrt(lax.optimization_barrier(jnp.mean(residual * residual, axis=1, keepdims=True)) + norm_eps)
    normed = (scaled * norm_gain.astype(jnp.float32)).astype(jnp.bfloat16)
    flat_routes = routes.reshape(-1).astype(jnp.int32)
    flat_rows = jnp.repeat(normed, TOPK, axis=0)
    buffer_rows = N_SP * N_TP * CAP
    quarter = EXPERT_FF // N_TP

    def per_expert(carry, expert):
        chosen = flat_routes == expert
        rank = (jnp.cumsum(chosen.astype(jnp.int32)) - 1).astype(jnp.int32)
        place = jnp.where(chosen, rank, buffer_rows).astype(jnp.int32)
        buffer = jnp.zeros((buffer_rows, D), jnp.bfloat16).at[place].set(flat_rows, mode='drop')
        gate = jnp.dot(buffer, expert_gate[expert], preferred_element_type=jnp.float32)
        up_value = jnp.dot(buffer, expert_up[expert], preferred_element_type=jnp.float32)
        hidden = (jax.nn.silu(gate) * up_value).astype(jnp.bfloat16)
        down_w = expert_down[expert]
        output = jnp.zeros((buffer_rows, D), jnp.float32)
        for lane in range(N_TP):
            partial_out = jnp.dot(hidden[:, lane * quarter:(lane + 1) * quarter], down_w[lane * quarter:(lane + 1) * quarter], preferred_element_type=jnp.float32)
            output = output + lax.optimization_barrier(partial_out.astype(jnp.bfloat16)).astype(jnp.float32)
        picked = jnp.take(output, jnp.minimum(place, buffer_rows - 1), axis=0)
        return (carry + jnp.where(chosen[:, None], picked, jnp.float32(0.0)), None)
    routed, _ = lax.scan(per_expert, jnp.zeros((TOKENS * TOPK, D), jnp.float32), jnp.arange(EXPERTS, dtype=jnp.int32))
    moe = lax.optimization_barrier(jnp.sum(routed.reshape(TOKENS, TOPK, D) * route_weight.astype(jnp.float32)[:, :, None], axis=1))
    return (residual + moe).astype(jnp.bfloat16)
```

```python
import functools

import jax
import jax.numpy as jnp
from jax import lax
from jax.experimental import pallas as pl
from jax.experimental.pallas import tpu as pltpu
from jax.sharding import PartitionSpec as P

MESH = pl.DeviceIdType.MESH
BF16 = jnp.bfloat16
F32 = jnp.float32
I32 = jnp.int32

norm_eps = 1e-06
PAIR = 2
SEG = 256
HALO = 16


def iota(shape, dim):
    return lax.broadcasted_iota(I32, shape, dim)


def dot(a, b):
    return jnp.dot(a, b, preferred_element_type=F32)


def settle(like, sem):
    pltpu.make_async_copy(like, like, sem).wait()


def kernel(
    sizes,
    resid_ref,
    pool_ref,
    map_ref,
    scale_ref,
    proj_ref,
    gain_ref,
    routes_ref,
    weight_ref,
    gate_hbm,
    up_hbm,
    down_hbm,
    out_ref,
    ext,
    halo,
    pieces,
    piece_in,
    proj_in,
    mixed,
    spread,
    gather,
    w_hi,
    w_lo,
    w_gu,
    w_down,
    stack,
    go,
    came,
    rows,
    hidden,
    part,
    part_in,
    back,
    home,
    total,
    w_sem,
    halo_sem,
    proj_send,
    proj_recv,
    mate_send,
    mate_recv,
    piece_send,
    piece_recv,
    go_send,
    go_recv,
    row_send,
    row_recv,
    part_send,
    part_recv,
    back_send,
    back_recv,
):
    n, lanes, chunks, slots = sizes
    tokens, width = resid_ref.shape
    seq_rows, gdim = pool_ref.shape
    segs = width // SEG
    block = PAIR * segs
    crows = PAIR * n
    half = gdim // 2
    me = lax.axis_index("sp")
    lane = lax.axis_index("tp")
    core = lax.rem(me, 2)
    mate = me + 1 - 2 * core

    def sp_at(k):
        return lax.rem(me + k, n)

    def tp_at(k):
        return lax.rem(lane + k, lanes)

    def remote(src, dst, send, recv, where):
        return pltpu.make_async_remote_copy(
            src_ref=src,
            dst_ref=dst,
            send_sem=send,
            recv_sem=recv,
            device_id=where,
            device_id_type=MESH,
        )

    barrier = pltpu.get_barrier_semaphore()

    def greet(k, carry):
        pl.semaphore_signal(
            barrier, inc=1, device_id={"sp": sp_at(k)}, device_id_type=MESH
        )
        return carry

    lax.fori_loop(1, n, greet, 0)
    for k in range(1, lanes):
        pl.semaphore_signal(
            barrier, inc=1, device_id={"tp": tp_at(k)}, device_id_type=MESH
        )

    size = n * block
    a, b = iota((size, size), 0), iota((size, size), 1)
    seg_a, rest = a // crows, lax.rem(a, crows)
    where = (rest // PAIR) * block + seg_a * PAIR + lax.rem(rest, PAIR)
    gather[...] = (b == where).astype(F32).astype(BF16)
    seg_b, rest_b = b // crows, lax.rem(b, crows)
    where_b = (rest_b // PAIR) * block + seg_b * PAIR + lax.rem(rest_b, PAIR)
    spread[...] = (a == where_b).astype(F32).astype(BF16)

    one0 = (iota((n, tokens), 0) == routes_ref[0:1, :]).astype(F32)
    one1 = (iota((n, tokens), 0) == routes_ref[1:2, :]).astype(F32)
    before = (iota((tokens, tokens), 0) < iota((tokens, tokens), 1)).astype(F32).astype(BF16)
    rank0 = dot(one0.astype(BF16), before)
    rank1 = dot(one1.astype(BF16), before) + jnp.sum(one0, axis=1, keepdims=True)
    slot0 = jnp.sum(rank0 * one0, axis=0, keepdims=True).astype(I32)
    slot1 = jnp.sum(rank1 * one1, axis=0, keepdims=True).astype(I32)
    row0 = (slot0 // PAIR) * crows + routes_ref[0:1, :] * PAIR + lax.rem(slot0, PAIR)
    row1 = (slot1 // PAIR) * crows + routes_ref[1:2, :] * PAIR + lax.rem(slot1, PAIR)
    place = iota((chunks * crows, tokens), 0)
    hit0, hit1 = place == row0, place == row1
    weight = jnp.where(hit0, weight_ref[0:1, :], 0.0) + jnp.where(hit1, weight_ref[1:2, :], 0.0)
    high = weight.astype(BF16)
    w_hi[...] = high.reshape(chunks, crows, tokens)
    w_lo[...] = (weight - high.astype(F32)).astype(BF16).reshape(chunks, crows, tokens)
    placing = (jnp.where(hit0, 1.0, 0.0) + jnp.where(hit1, 1.0, 0.0)).astype(BF16)

    pl.semaphore_wait(barrier, n - 1 + lanes - 1)

    halo_copy = remote(
        pool_ref.at[pl.ds(seq_rows - HALO, HALO)],
        halo,
        halo_sem.at[0],
        halo_sem.at[1],
        {"sp": sp_at(1)},
    )
    halo_copy.start()
    mine = pl.ds(pl.multiple_of(core * half, half), half)
    other = pl.ds(pl.multiple_of((1 - core) * half, half), half)

    def proj_copy(k):
        return remote(
            proj_ref.at[mine],
            proj_in.at[k - 1, mine],
            proj_send.at[k - 1],
            proj_recv.at[k - 1],
            {"tp": tp_at(k)},
        )

    def mate_copy(k):
        return remote(
            proj_in.at[k - 1, mine],
            proj_in.at[k - 1, mine],
            mate_send.at[k - 1],
            mate_recv.at[k - 1],
            {"sp": mate},
        )

    order = [k for k in (1, 3, 2) if k < lanes]
    for k in order:
        proj_copy(k).start()

    tiles = w_gu.shape[0]
    cols = w_down.shape[0]
    tile = w_gu.shape[2] // 2

    def weight_copies():
        found = []
        for i in range(tiles):
            for j, source in enumerate((gate_hbm, up_hbm)):
                found.append(
                    pltpu.make_async_copy(
                        source.at[0, :, pl.ds(i * tile, tile)],
                        w_gu.at[i, :, pl.ds(j * tile, tile)],
                        w_sem.at[j * tiles + i],
                    )
                )
        for i in range(cols):
            found.append(
                pltpu.make_async_copy(
                    down_hbm.at[0, :, pl.ds(i * SEG, SEG)], w_down.at[i], w_sem.at[2 * tiles + i]
                )
            )
        return found

    for copy in weight_copies():
        copy.start()

    ext[pl.ds(HALO, seq_rows)] = pool_ref[...].astype(F32)
    halo_copy.wait()
    ext[pl.ds(0, HALO)] = jnp.where(me > 0, halo[...].astype(F32), 0.0)
    span = seq_rows + HALO
    levels = []
    reach = 1
    for level in range(lanes):
        kept = ext[pl.ds(0, span)]
        ext[pl.ds(reach, span - reach)] = kept[reach:] + kept[: span - reach]
        levels.append(ext[pl.ds(HALO, seq_rows)])
        reach *= 2
    window_sum = levels[0]
    for level in range(1, lanes):
        window_sum = jnp.where(lane == level, levels[level], window_sum)
    window = jnp.left_shift(jnp.int32(2), lane)
    positions = me * seq_rows + 1 + iota((seq_rows, gdim), 0)
    divisor = jnp.minimum(positions, window).astype(F32)
    pooled = (window_sum / divisor - pool_ref[...].astype(F32)).astype(BF16)
    pieces[...] = (dot(pooled, map_ref[0]) * scale_ref[...].astype(F32)).astype(BF16)

    def piece_copy(k):
        return remote(
            pieces.at[pl.ds(pl.multiple_of(tp_at(k) * tokens, tokens), tokens)],
            piece_in.at[k - 1],
            piece_send.at[k - 1],
            piece_recv.at[k - 1],
            {"tp": tp_at(k)},
        )

    for k in order:
        piece_copy(k).start()
    mix = dot(pieces[pl.ds(pl.multiple_of(lane * tokens, tokens), tokens)], proj_ref[...])
    for k in order:
        proj_copy(k).wait_recv()
        mate_copy(k).start()
    for k in order:
        piece_copy(k).wait_recv()
        settle(proj_in.at[k - 1, other], mate_recv.at[k - 1])
        mix = mix + dot(piece_in[k - 1], proj_in[k - 1])
    mixed_value = (resid_ref[...].astype(F32) + mix).astype(BF16)
    mixed[...] = mixed_value
    residual = mixed_value.astype(F32)
    scaled = residual * lax.rsqrt(
        jnp.sum(residual * residual, axis=1, keepdims=True) / width + norm_eps
    )
    normed = (scaled * gain_ref[...].astype(F32)).astype(BF16)
    routed = dot(placing, normed).astype(BF16)
    total[...] = residual

    def to_blocks(value, target):
        for s in range(segs):
            stack[pl.ds(s * crows, crows)] = value[:, s * SEG : (s + 1) * SEG]
        target[...] = dot(spread[...], stack[...]).astype(BF16)

    for c in range(chunks):
        to_blocks(routed[c * crows : (c + 1) * crows], go.at[c])

    def send_blocks(source, target, c, send, recv):
        own = pl.ds(pl.multiple_of(me * block, block), block)

        def one(k, carry):
            to = sp_at(k)
            remote(
                source.at[c, pl.ds(pl.multiple_of(to * block, block), block)],
                target.at[c, own],
                send.at[c],
                recv.at[c],
                {"sp": to},
            ).start()
            return carry

        def both(k, carry):
            one(k, 0)
            one(n - k, 0)
            return carry

        lax.fori_loop(1, n // 2, both, 0)
        one(n // 2, 0)

    def take_blocks(source, target, c, recv):
        own = pl.ds(pl.multiple_of(me * block, block), block)
        settle(target.at[c, pl.ds(0, (n - 1) * block)], recv.at[c])
        target[c, own] = source[c, own]
        return dot(gather[...], target[c]).astype(BF16)

    def row_copy(c, k):
        own = pl.ds(pl.multiple_of(lane * crows, crows), crows)
        return remote(
            rows.at[c, own],
            rows.at[c, own],
            row_send.at[c, k - 1],
            row_recv.at[c, k - 1],
            {"tp": tp_at(k)},
        )

    def part_copy(c, k):
        theirs = pl.ds(pl.multiple_of(tp_at(k) * crows, crows), crows)
        return remote(
            part.at[c, theirs],
            part_in.at[c, k - 1],
            part_send.at[c, k - 1],
            part_recv.at[c, k - 1],
            {"tp": tp_at(k)},
        )

    ahead = min(2, chunks)
    for c in range(ahead):
        send_blocks(go, came, c, go_send, go_recv)
    for copy in weight_copies():
        copy.wait()

    def step(k, carry):
        @pl.when(k < chunks)
        def _():
            flat = take_blocks(go, came, k, go_recv)
            own = pl.ds(pl.multiple_of(lane * crows, crows), crows)
            for s in range(segs):
                rows[k, own, s * SEG : (s + 1) * SEG] = flat[s * crows : (s + 1) * crows]
            for j in order:
                row_copy(k, j).start()

            @pl.when(k + ahead < chunks)
            def _():
                send_blocks(go, came, k + ahead, go_send, go_recv)

        @pl.when((k >= 1) & (k < chunks + 1))
        def _():
            c = k - 1
            for j in order:
                row_copy(c, j).wait_recv()

            def up_tile(i, carry):
                both = dot(rows[c], w_gu[i])
                g, u = both[:, :tile], both[:, tile:]
                hidden[:, pl.ds(pl.multiple_of(i * tile, tile), tile)] = (
                    (g / (1.0 + jnp.exp(-g))) * u
                ).astype(BF16)
                return carry

            lax.fori_loop(0, tiles, up_tile, 0)

            def down_tile(i, carry):
                part[c, :, pl.ds(pl.multiple_of(i * SEG, SEG), SEG)] = dot(
                    hidden[...], w_down[i]
                ).astype(BF16)
                return carry

            lax.fori_loop(0, cols, down_tile, 0)
            for j in order:
                part_copy(c, j).start()

        @pl.when((k >= 2) & (k < chunks + 2))
        def _():
            c = k - 2
            own = pl.ds(pl.multiple_of(lane * crows, crows), crows)
            for j in order:
                part_copy(c, j).wait_recv()
            value = part[c, own].astype(F32)
            for j in order:
                value = value + part_in[c, j - 1].astype(F32)
            to_blocks(value.astype(BF16), back.at[c])
            send_blocks(back, home, c, back_send, back_recv)

        @pl.when(k >= 3)
        def _():
            c = k - 3
            flat = take_blocks(back, home, c, back_recv)
            sides = (((0,), (0,)), ((), ()))
            for s in range(segs):
                piece = flat[s * crows : (s + 1) * crows]
                cut = pl.ds(s * SEG, SEG)
                total[:, cut] += lax.dot_general(
                    w_hi[c], piece, sides, preferred_element_type=F32
                ) + lax.dot_general(w_lo[c], piece, sides, preferred_element_type=F32)

        return carry

    lax.fori_loop(0, chunks + 3, step, 0)
    out_ref[...] = total[...].astype(BF16)

    for k in order:
        proj_copy(k).wait_send()
        mate_copy(k).wait_send()
        piece_copy(k).wait_send()

    def drain(c, carry):
        settle(go.at[c, pl.ds(0, (n - 1) * block)], go_send.at[c])
        settle(back.at[c, pl.ds(0, (n - 1) * block)], back_send.at[c])
        for k in order:
            row_copy(c, k).wait_send()
            part_copy(c, k).wait_send()
        return carry

    lax.fori_loop(0, chunks, drain, 0)


def local(
    resid,
    pool_input,
    group_map,
    pool_scale,
    out_proj,
    norm_gain,
    routes,
    route_weight,
    expert_gate,
    expert_up,
    expert_down,
):
    n, lanes = lax.axis_size("sp"), lax.axis_size("tp")
    tokens, width = resid.shape
    seq_rows, gdim = pool_input.shape
    ff = expert_gate.shape[2]
    slots = max(2, 5 * tokens * routes.shape[1] // (4 * n))
    chunks = slots // PAIR
    assert chunks * PAIR == slots
    segs = width // SEG
    size = n * PAIR * segs
    crows = PAIR * n
    tile = min(128, ff)
    tiles, cols = ff // tile, width // SEG
    vmem, dma = pltpu.VMEM, pltpu.SemaphoreType.DMA
    hbm = pl.BlockSpec(memory_space=pl.ANY)
    scratch = [
        vmem((HALO + seq_rows, gdim), F32),
        vmem((HALO, gdim), BF16),
        vmem((seq_rows, gdim), BF16),
        vmem((lanes - 1, tokens, gdim), BF16),
        vmem((lanes - 1, gdim, width), BF16),
        vmem((tokens, width), BF16),
        vmem((size, size), BF16),
        vmem((size, size), BF16),
        vmem((chunks, crows, tokens), BF16),
        vmem((chunks, crows, tokens), BF16),
        vmem((tiles, width, 2 * tile), BF16),
        vmem((cols, ff, SEG), BF16),
        vmem((size, SEG), BF16),
        vmem((chunks, size, SEG), BF16),
        vmem((chunks, size, SEG), BF16),
        vmem((chunks, lanes * crows, width), BF16),
        vmem((lanes * crows, ff), BF16),
        vmem((chunks, lanes * crows, width), BF16),
        vmem((chunks, lanes - 1, crows, width), BF16),
        vmem((chunks, size, SEG), BF16),
        vmem((chunks, size, SEG), BF16),
        vmem((tokens, width), F32),
        dma((2 * tiles + cols,)),
        dma((2,)),
        dma((lanes - 1,)),
        dma((lanes - 1,)),
        dma((lanes - 1,)),
        dma((lanes - 1,)),
        dma((lanes - 1,)),
        dma((lanes - 1,)),
        dma((chunks,)),
        dma((chunks,)),
        dma((chunks, lanes - 1)),
        dma((chunks, lanes - 1)),
        dma((chunks, lanes - 1)),
        dma((chunks, lanes - 1)),
        dma((chunks,)),
        dma((chunks,)),
    ]
    return pl.pallas_call(
        functools.partial(kernel, (n, lanes, chunks, slots)),
        out_shape=jax.ShapeDtypeStruct((tokens, width), BF16),
        in_specs=[pl.BlockSpec(memory_space=vmem)] * 8 + [hbm] * 3,
        out_specs=pl.BlockSpec(memory_space=vmem),
        scratch_shapes=scratch,
        compiler_params=pltpu.CompilerParams(
            collective_id=0, has_side_effects=True, vmem_limit_bytes=60 * 1024 * 1024
        ),
        name="layer",
    )(
        resid,
        pool_input,
        group_map,
        pool_scale.reshape(1, -1),
        out_proj,
        norm_gain.reshape(1, -1),
        routes.T,
        route_weight.T,
        expert_gate,
        expert_up,
        expert_down,
    )


def solution(mesh):
    return jax.shard_map(
        local,
        mesh=mesh,
        in_specs=(
            P(("grp", "sp", "tp"), None),
            P(("grp", "sp"), "tp"),
            P("tp", None, None),
            P("tp"),
            P("tp", None),
            P(),
            P(("grp", "sp", "tp"), None),
            P(("grp", "sp", "tp"), None),
            P("sp", None, "tp"),
            P("sp", None, "tp"),
            P("sp", "tp", None),
        ),
        out_specs=P(("grp", "sp", "tp"), None),
        check_vma=False,
    )
```

```python
import functools

import jax
import jax.numpy as jnp
from jax import lax
from jax.experimental import pallas as pl
from jax.experimental.pallas import tpu as pltpu
from jax.sharding import PartitionSpec as P

MESH = pl.DeviceIdType.MESH
BF16 = jnp.bfloat16
F32 = jnp.float32
I32 = jnp.int32

norm_eps = 1e-06
PAIR = 2
SEG = 256
HALO = 16
AHEAD = 2

SCHEDULE = (
    ("arrive", 0),
    ("send_next", -AHEAD),
    ("experts", 1),
    ("relay", 0),
    ("add_far", 1),
    ("give_back", 2),
    ("combine", 3),
)


def iota(shape, dim):
    return lax.broadcasted_iota(I32, shape, dim)


def dot(a, b):
    return jnp.dot(a, b, preferred_element_type=F32)


def settle(like, sem):
    pltpu.make_async_copy(like, like, sem).wait()


def kernel(
    sizes,
    resid_ref,
    pool_ref,
    map_ref,
    scale_ref,
    proj_ref,
    gain_ref,
    routes_ref,
    weight_ref,
    gate_hbm,
    up_hbm,
    down_hbm,
    out_ref,
    ext,
    halo,
    pieces,
    piece_in,
    proj_in,
    mixed,
    spread,
    gather,
    w_hi,
    w_lo,
    w_gu,
    w_down,
    stack,
    go,
    came,
    rows,
    hidden,
    part,
    part_in,
    far_in,
    back,
    home,
    total,
    w_sem,
    halo_sem,
    proj_send,
    proj_recv,
    mate_send,
    mate_recv,
    piece_send,
    piece_recv,
    go_send,
    go_recv,
    row_send,
    row_recv,
    part_send,
    part_recv,
    back_send,
    back_recv,
):
    n, lanes, chunks, slots = sizes
    tokens, width = resid_ref.shape
    seq_rows, gdim = pool_ref.shape
    segs = width // SEG
    block = PAIR * segs
    crows = PAIR * n
    half = gdim // 2
    me = lax.axis_index("sp")
    lane = lax.axis_index("tp")
    core = lax.rem(me, 2)
    mate = me + 1 - 2 * core

    def sp_at(k):
        return lax.rem(me + k, n)

    def tp_at(k):
        return lax.rem(lane + k, lanes)

    def remote(src, dst, send, recv, where):
        return pltpu.make_async_remote_copy(
            src_ref=src,
            dst_ref=dst,
            send_sem=send,
            recv_sem=recv,
            device_id=where,
            device_id_type=MESH,
        )

    barrier = pltpu.get_barrier_semaphore()

    def greet(k, carry):
        pl.semaphore_signal(
            barrier, inc=1, device_id={"sp": sp_at(k)}, device_id_type=MESH
        )
        return carry

    lax.fori_loop(1, n, greet, 0)
    for k in range(1, lanes):
        pl.semaphore_signal(
            barrier, inc=1, device_id={"tp": tp_at(k)}, device_id_type=MESH
        )

    size = n * block
    a, b = iota((size, size), 0), iota((size, size), 1)
    seg_a, rest = a // crows, lax.rem(a, crows)
    where = (rest // PAIR) * block + seg_a * PAIR + lax.rem(rest, PAIR)
    gather[...] = (b == where).astype(F32).astype(BF16)
    seg_b, rest_b = b // crows, lax.rem(b, crows)
    where_b = (rest_b // PAIR) * block + seg_b * PAIR + lax.rem(rest_b, PAIR)
    spread[...] = (a == where_b).astype(F32).astype(BF16)

    one0 = (iota((n, tokens), 0) == routes_ref[0:1, :]).astype(F32)
    one1 = (iota((n, tokens), 0) == routes_ref[1:2, :]).astype(F32)
    before = (iota((tokens, tokens), 0) < iota((tokens, tokens), 1)).astype(F32).astype(BF16)
    rank0 = dot(one0.astype(BF16), before)
    rank1 = dot(one1.astype(BF16), before) + jnp.sum(one0, axis=1, keepdims=True)
    slot0 = jnp.sum(rank0 * one0, axis=0, keepdims=True).astype(I32)
    slot1 = jnp.sum(rank1 * one1, axis=0, keepdims=True).astype(I32)
    row0 = (slot0 // PAIR) * crows + routes_ref[0:1, :] * PAIR + lax.rem(slot0, PAIR)
    row1 = (slot1 // PAIR) * crows + routes_ref[1:2, :] * PAIR + lax.rem(slot1, PAIR)
    place = iota((chunks * crows, tokens), 0)
    hit0, hit1 = place == row0, place == row1
    weight = jnp.where(hit0, weight_ref[0:1, :], 0.0) + jnp.where(hit1, weight_ref[1:2, :], 0.0)
    high = weight.astype(BF16)
    w_hi[...] = high.reshape(chunks, crows, tokens)
    w_lo[...] = (weight - high.astype(F32)).astype(BF16).reshape(chunks, crows, tokens)
    placing = (jnp.where(hit0, 1.0, 0.0) + jnp.where(hit1, 1.0, 0.0)).astype(BF16)

    pl.semaphore_wait(barrier, n - 1 + lanes - 1)

    halo_copy = remote(
        pool_ref.at[pl.ds(seq_rows - HALO, HALO)],
        halo,
        halo_sem.at[0],
        halo_sem.at[1],
        {"sp": sp_at(1)},
    )
    halo_copy.start()
    mine = pl.ds(pl.multiple_of(core * half, half), half)
    other = pl.ds(pl.multiple_of((1 - core) * half, half), half)

    def proj_copy(k):
        return remote(
            proj_ref.at[mine],
            proj_in.at[k - 1, mine],
            proj_send.at[k - 1],
            proj_recv.at[k - 1],
            {"tp": tp_at(k)},
        )

    def mate_copy(k):
        return remote(
            proj_in.at[k - 1, mine],
            proj_in.at[k - 1, mine],
            mate_send.at[k - 1],
            mate_recv.at[k - 1],
            {"sp": mate},
        )

    order = [k for k in (1, 3, 2) if k < lanes]
    for k in order:
        proj_copy(k).start()

    tiles = w_gu.shape[0]
    cols = w_down.shape[0]
    tile = w_gu.shape[2] // 2

    def weight_copies():
        found = []
        for i in range(tiles):
            for j, source in enumerate((gate_hbm, up_hbm)):
                found.append(
                    pltpu.make_async_copy(
                        source.at[0, :, pl.ds(i * tile, tile)],
                        w_gu.at[i, :, pl.ds(j * tile, tile)],
                        w_sem.at[j * tiles + i],
                    )
                )
        for i in range(cols):
            found.append(
                pltpu.make_async_copy(
                    down_hbm.at[0, :, pl.ds(i * SEG, SEG)], w_down.at[i], w_sem.at[2 * tiles + i]
                )
            )
        return found

    for copy in weight_copies():
        copy.start()

    ext[pl.ds(HALO, seq_rows)] = pool_ref[...].astype(F32)
    halo_copy.wait()
    ext[pl.ds(0, HALO)] = jnp.where(me > 0, halo[...].astype(F32), 0.0)
    span = seq_rows + HALO
    levels = []
    reach = 1
    for level in range(lanes):
        kept = ext[pl.ds(0, span)]
        ext[pl.ds(reach, span - reach)] = kept[reach:] + kept[: span - reach]
        levels.append(ext[pl.ds(HALO, seq_rows)])
        reach *= 2
    window_sum = levels[0]
    for level in range(1, lanes):
        window_sum = jnp.where(lane == level, levels[level], window_sum)
    window = jnp.left_shift(jnp.int32(2), lane)
    positions = me * seq_rows + 1 + iota((seq_rows, gdim), 0)
    divisor = jnp.minimum(positions, window).astype(F32)
    pooled = (window_sum / divisor - pool_ref[...].astype(F32)).astype(BF16)
    pieces[...] = (dot(pooled, map_ref[0]) * scale_ref[...].astype(F32)).astype(BF16)

    def piece_copy(k):
        return remote(
            pieces.at[pl.ds(pl.multiple_of(tp_at(k) * tokens, tokens), tokens)],
            piece_in.at[k - 1],
            piece_send.at[k - 1],
            piece_recv.at[k - 1],
            {"tp": tp_at(k)},
        )

    for k in order:
        piece_copy(k).start()
    mix = dot(pieces[pl.ds(pl.multiple_of(lane * tokens, tokens), tokens)], proj_ref[...])
    for k in order:
        proj_copy(k).wait_recv()
        mate_copy(k).start()
    for k in order:
        piece_copy(k).wait_recv()
        settle(proj_in.at[k - 1, other], mate_recv.at[k - 1])
        mix = mix + dot(piece_in[k - 1], proj_in[k - 1])
    mixed_value = (resid_ref[...].astype(F32) + mix).astype(BF16)
    mixed[...] = mixed_value
    residual = mixed_value.astype(F32)
    scaled = residual * lax.rsqrt(
        jnp.sum(residual * residual, axis=1, keepdims=True) / width + norm_eps
    )
    normed = (scaled * gain_ref[...].astype(F32)).astype(BF16)
    routed = dot(placing, normed).astype(BF16)
    total[...] = residual

    def to_blocks(value, target):
        for s in range(segs):
            stack[pl.ds(s * crows, crows)] = value[:, s * SEG : (s + 1) * SEG]
        target[...] = dot(spread[...], stack[...]).astype(BF16)

    for c in range(chunks):
        to_blocks(routed[c * crows : (c + 1) * crows], go.at[c])

    def send_blocks(source, target, c, send, recv):
        own = pl.ds(pl.multiple_of(me * block, block), block)

        def one(k, carry):
            to = sp_at(k)
            remote(
                source.at[c, pl.ds(pl.multiple_of(to * block, block), block)],
                target.at[c, own],
                send.at[c],
                recv.at[c],
                {"sp": to},
            ).start()
            return carry

        def both(k, carry):
            one(k, 0)
            one(n - k, 0)
            return carry

        lax.fori_loop(1, n // 2, both, 0)
        one(n // 2, 0)

    def take_blocks(source, target, c, recv):
        own = pl.ds(pl.multiple_of(me * block, block), block)
        settle(target.at[c, pl.ds(0, (n - 1) * block)], recv.at[c])
        target[c, own] = source[c, own]
        return dot(gather[...], target[c]).astype(BF16)

    right, left = {"tp": tp_at(1)}, {"tp": tp_at(lanes - 1)}
    low = crows // 2

    def of_lane(k, start, count):
        return pl.ds(pl.multiple_of(tp_at(k) * crows + start, low), count)

    def row_copies(c):
        def one(k, start, i, to):
            at = rows.at[c, of_lane(k, start, low)]
            return remote(at, at, row_send.at[c, i], row_recv.at[c, i], to)

        return (
            one(0, 0, 0, right),
            one(0, low, 1, left),
            one(0, low, 2, right),
            one(0, 0, 3, left),
            one(lanes - 1, 0, 4, right),
            one(1, low, 5, left),
        )

    def part_copies(c):
        def one(k, start, target, i, to):
            at = part.at[c, of_lane(k, start, low)]
            return remote(at, target, part_send.at[c, i], part_recv.at[c, i], to)

        return (
            one(2, 0, far_in.at[c, 0], 0, right),
            one(2, low, far_in.at[c, 1], 1, left),
            one(1, low, part_in.at[c, 0, pl.ds(low, low)], 2, right),
            one(lanes - 1, 0, part_in.at[c, 1, pl.ds(0, low)], 3, left),
            one(1, 0, part_in.at[c, 0, pl.ds(0, low)], 4, right),
            one(lanes - 1, low, part_in.at[c, 1, pl.ds(low, low)], 5, left),
        )

    ahead = min(AHEAD, chunks)
    for c in range(ahead):
        send_blocks(go, came, c, go_send, go_recv)
    for copy in weight_copies():
        copy.wait()

    def arrive(c):
        flat = take_blocks(go, came, c, go_recv)
        own = of_lane(0, 0, crows)
        for s in range(segs):
            rows[c, own, s * SEG : (s + 1) * SEG] = flat[s * crows : (s + 1) * crows]
        for copy in row_copies(c)[:4]:
            copy.start()

    def relay(c):
        copies = row_copies(c)
        for i in (0, 1):
            copies[i].wait_recv()
            copies[4 + i].start()

    def experts(c):
        copies = row_copies(c)
        for i in (2, 3, 4, 5):
            copies[i].wait_recv()

        def up_tile(i, carry):
            both = dot(rows[c], w_gu[i])
            g, u = both[:, :tile], both[:, tile:]
            hidden[:, pl.ds(pl.multiple_of(i * tile, tile), tile)] = (
                (g / (1.0 + jnp.exp(-g))) * u
            ).astype(BF16)
            return carry

        lax.fori_loop(0, tiles, up_tile, 0)

        def down_tile(i, carry):
            part[c, :, pl.ds(pl.multiple_of(i * SEG, SEG), SEG)] = dot(
                hidden[...], w_down[i]
            ).astype(BF16)
            return carry

        lax.fori_loop(0, cols, down_tile, 0)
        for copy in part_copies(c)[:4]:
            copy.start()

    def add_far(c):
        copies = part_copies(c)
        for i, (k, start) in enumerate(((1, 0), (lanes - 1, low))):
            copies[i].wait_recv()
            at = of_lane(k, start, low)
            part[c, at] = (part[c, at].astype(F32) + far_in[c, i].astype(F32)).astype(BF16)
            copies[4 + i].start()

    def give_back(c):
        copies = part_copies(c)
        for i in (2, 3, 4, 5):
            copies[i].wait_recv()
        value = part[c, of_lane(0, 0, crows)].astype(F32)
        value = value + part_in[c, 0].astype(F32) + part_in[c, 1].astype(F32)
        to_blocks(value.astype(BF16), back.at[c])
        send_blocks(back, home, c, back_send, back_recv)

    def combine(c):
        flat = take_blocks(back, home, c, back_recv)
        sides = (((0,), (0,)), ((), ()))
        for s in range(segs):
            piece = flat[s * crows : (s + 1) * crows]
            cut = pl.ds(s * SEG, SEG)
            total[:, cut] += lax.dot_general(
                w_hi[c], piece, sides, preferred_element_type=F32
            ) + lax.dot_general(w_lo[c], piece, sides, preferred_element_type=F32)

    def send_next(c):
        send_blocks(go, came, c, go_send, go_recv)

    stages = {
        "arrive": arrive,
        "relay": relay,
        "experts": experts,
        "add_far": add_far,
        "give_back": give_back,
        "combine": combine,
        "send_next": send_next,
    }

    def step(k, carry):
        for name, lag in SCHEDULE:
            c = k - lag
            low_end = ahead if name == "send_next" else 0

            @pl.when((c >= low_end) & (c < chunks))
            def _():
                stages[name](c)

        return carry

    lax.fori_loop(0, chunks + max(lag for _, lag in SCHEDULE), step, 0)
    out_ref[...] = total[...].astype(BF16)

    for k in order:
        proj_copy(k).wait_send()
        mate_copy(k).wait_send()
        piece_copy(k).wait_send()

    def drain(c, carry):
        settle(go.at[c, pl.ds(0, (n - 1) * block)], go_send.at[c])
        settle(back.at[c, pl.ds(0, (n - 1) * block)], back_send.at[c])
        for copy in row_copies(c) + part_copies(c):
            copy.wait_send()
        return carry

    lax.fori_loop(0, chunks, drain, 0)


def local(
    resid,
    pool_input,
    group_map,
    pool_scale,
    out_proj,
    norm_gain,
    routes,
    route_weight,
    expert_gate,
    expert_up,
    expert_down,
):
    n, lanes = lax.axis_size("sp"), lax.axis_size("tp")
    tokens, width = resid.shape
    seq_rows, gdim = pool_input.shape
    ff = expert_gate.shape[2]
    slots = max(2, 5 * tokens * routes.shape[1] // (4 * n))
    chunks = slots // PAIR
    assert chunks * PAIR == slots and lanes == 4
    segs = width // SEG
    size = n * PAIR * segs
    crows = PAIR * n
    tile = min(128, ff)
    tiles, cols = ff // tile, width // SEG
    vmem, dma = pltpu.VMEM, pltpu.SemaphoreType.DMA
    hbm = pl.BlockSpec(memory_space=pl.ANY)
    scratch = [
        vmem((HALO + seq_rows, gdim), F32),
        vmem((HALO, gdim), BF16),
        vmem((seq_rows, gdim), BF16),
        vmem((lanes - 1, tokens, gdim), BF16),
        vmem((lanes - 1, gdim, width), BF16),
        vmem((tokens, width), BF16),
        vmem((size, size), BF16),
        vmem((size, size), BF16),
        vmem((chunks, crows, tokens), BF16),
        vmem((chunks, crows, tokens), BF16),
        vmem((tiles, width, 2 * tile), BF16),
        vmem((cols, ff, SEG), BF16),
        vmem((size, SEG), BF16),
        vmem((chunks, size, SEG), BF16),
        vmem((chunks, size, SEG), BF16),
        vmem((chunks, lanes * crows, width), BF16),
        vmem((lanes * crows, ff), BF16),
        vmem((chunks, lanes * crows, width), BF16),
        vmem((chunks, 2, crows, width), BF16),
        vmem((chunks, 2, crows // 2, width), BF16),
        vmem((chunks, size, SEG), BF16),
        vmem((chunks, size, SEG), BF16),
        vmem((tokens, width), F32),
        dma((2 * tiles + cols,)),
        dma((2,)),
        dma((lanes - 1,)),
        dma((lanes - 1,)),
        dma((lanes - 1,)),
        dma((lanes - 1,)),
        dma((lanes - 1,)),
        dma((lanes - 1,)),
        dma((chunks,)),
        dma((chunks,)),
        dma((chunks, 6)),
        dma((chunks, 6)),
        dma((chunks, 6)),
        dma((chunks, 6)),
        dma((chunks,)),
        dma((chunks,)),
    ]
    return pl.pallas_call(
        functools.partial(kernel, (n, lanes, chunks, slots)),
        out_shape=jax.ShapeDtypeStruct((tokens, width), BF16),
        in_specs=[pl.BlockSpec(memory_space=vmem)] * 8 + [hbm] * 3,
        out_specs=pl.BlockSpec(memory_space=vmem),
        scratch_shapes=scratch,
        compiler_params=pltpu.CompilerParams(
            collective_id=0, has_side_effects=True, vmem_limit_bytes=60 * 1024 * 1024
        ),
        name="layer",
    )(
        resid,
        pool_input,
        group_map,
        pool_scale.reshape(1, -1),
        out_proj,
        norm_gain.reshape(1, -1),
        routes.T,
        route_weight.T,
        expert_gate,
        expert_up,
        expert_down,
    )


def solution(mesh):
    return jax.shard_map(
        local,
        mesh=mesh,
        in_specs=(
            P(("grp", "sp", "tp"), None),
            P(("grp", "sp"), "tp"),
            P("tp", None, None),
            P("tp"),
            P("tp", None),
            P(),
            P(("grp", "sp", "tp"), None),
            P(("grp", "sp", "tp"), None),
            P("sp", None, "tp"),
            P("sp", None, "tp"),
            P("sp", "tp", None),
        ),
        out_specs=P(("grp", "sp", "tp"), None),
        check_vma=False,
    )
```

```python
import functools

import jax
import jax.numpy as jnp
from jax import lax
from jax.experimental import pallas as pl
from jax.experimental.pallas import tpu as pltpu
from jax.sharding import PartitionSpec as P

MESH = pl.DeviceIdType.MESH
BF16 = jnp.bfloat16
F32 = jnp.float32
I32 = jnp.int32

norm_eps = 1e-06
PAIR = 2
SEG = 256
HALO = 16
AHEAD = 2

SCHEDULE = (
    ("arrive", 0),
    ("send_next", -AHEAD),
    ("experts", 1),
    ("relay", 0),
    ("add_far", 1),
    ("give_back", 2),
    ("combine", 3),
)


def iota(shape, dim):
    return lax.broadcasted_iota(I32, shape, dim)


def dot(a, b):
    return jnp.dot(a, b, preferred_element_type=F32)


def settle(like, sem):
    pltpu.make_async_copy(like, like, sem).wait()


def kernel(
    sizes,
    resid_ref,
    pool_ref,
    map_ref,
    scale_ref,
    proj_ref,
    gain_ref,
    routes_ref,
    weight_ref,
    gate_hbm,
    up_hbm,
    down_hbm,
    out_ref,
    ext,
    halo,
    pieces,
    piece_in,
    proj_in,
    mixed,
    spread,
    gather,
    w_hi,
    w_lo,
    w_gu,
    w_down,
    stack,
    go,
    came,
    rows,
    hidden,
    part,
    part_in,
    far_in,
    back,
    home,
    total,
    known,
    w_sem,
    halo_sem,
    proj_send,
    proj_recv,
    mate_send,
    mate_recv,
    piece_send,
    piece_recv,
    go_send,
    go_recv,
    row_send,
    row_recv,
    part_send,
    part_recv,
    back_send,
    back_recv,
):
    n, lanes, chunks, slots = sizes
    tokens, width = resid_ref.shape
    seq_rows, gdim = pool_ref.shape
    segs = width // SEG
    block = PAIR * segs
    crows = PAIR * n
    half = gdim // 2
    me = lax.axis_index("sp")
    lane = lax.axis_index("tp")
    core = lax.rem(me, 2)
    mate = me + 1 - 2 * core

    def sp_at(k):
        return lax.rem(me + k, n)

    def tp_at(k):
        return lax.rem(lane + k, lanes)

    def remote(src, dst, send, recv, where):
        return pltpu.make_async_remote_copy(
            src_ref=src,
            dst_ref=dst,
            send_sem=send,
            recv_sem=recv,
            device_id=where,
            device_id_type=MESH,
        )

    barrier = pltpu.get_barrier_semaphore()

    def greet(sem, radius):
        for k in (radius, n - radius):
            pl.semaphore_signal(
                sem, inc=1, device_id={"sp": sp_at(k)}, device_id_type=MESH
            )

    greet(barrier, 1)
    for k in range(1, lanes):
        pl.semaphore_signal(
            barrier, inc=1, device_id={"tp": tp_at(k)}, device_id_type=MESH
        )

    size = n * block
    a, b = iota((size, size), 0), iota((size, size), 1)
    seg_a, rest = a // crows, lax.rem(a, crows)
    where = (rest // PAIR) * block + seg_a * PAIR + lax.rem(rest, PAIR)
    gather[...] = (b == where).astype(F32).astype(BF16)
    seg_b, rest_b = b // crows, lax.rem(b, crows)
    where_b = (rest_b // PAIR) * block + seg_b * PAIR + lax.rem(rest_b, PAIR)
    spread[...] = (a == where_b).astype(F32).astype(BF16)

    one0 = (iota((n, tokens), 0) == routes_ref[0:1, :]).astype(F32)
    one1 = (iota((n, tokens), 0) == routes_ref[1:2, :]).astype(F32)
    before = (iota((tokens, tokens), 0) < iota((tokens, tokens), 1)).astype(F32).astype(BF16)
    rank0 = dot(one0.astype(BF16), before)
    rank1 = dot(one1.astype(BF16), before) + jnp.sum(one0, axis=1, keepdims=True)
    slot0 = jnp.sum(rank0 * one0, axis=0, keepdims=True).astype(I32)
    slot1 = jnp.sum(rank1 * one1, axis=0, keepdims=True).astype(I32)
    row0 = (slot0 // PAIR) * crows + routes_ref[0:1, :] * PAIR + lax.rem(slot0, PAIR)
    row1 = (slot1 // PAIR) * crows + routes_ref[1:2, :] * PAIR + lax.rem(slot1, PAIR)
    place = iota((chunks * crows, tokens), 0)
    hit0, hit1 = place == row0, place == row1
    weight = jnp.where(hit0, weight_ref[0:1, :], 0.0) + jnp.where(hit1, weight_ref[1:2, :], 0.0)
    high = weight.astype(BF16)
    w_hi[...] = high.reshape(chunks, crows, tokens)
    w_lo[...] = (weight - high.astype(F32)).astype(BF16).reshape(chunks, crows, tokens)
    placing = (jnp.where(hit0, 1.0, 0.0) + jnp.where(hit1, 1.0, 0.0)).astype(BF16)

    pl.semaphore_wait(barrier, 2 + lanes - 1)

    halo_copy = remote(
        pool_ref.at[pl.ds(seq_rows - HALO, HALO)],
        halo,
        halo_sem.at[0],
        halo_sem.at[1],
        {"sp": sp_at(1)},
    )
    halo_copy.start()
    mine = pl.ds(pl.multiple_of(core * half, half), half)
    other = pl.ds(pl.multiple_of((1 - core) * half, half), half)

    def proj_copy(k):
        return remote(
            proj_ref.at[mine],
            proj_in.at[k - 1, mine],
            proj_send.at[k - 1],
            proj_recv.at[k - 1],
            {"tp": tp_at(k)},
        )

    def mate_copy(k):
        return remote(
            proj_in.at[k - 1, mine],
            proj_in.at[k - 1, mine],
            mate_send.at[k - 1],
            mate_recv.at[k - 1],
            {"sp": mate},
        )

    order = [k for k in (1, 3, 2) if k < lanes]
    for k in order:
        proj_copy(k).start()

    radius, level = 1, 0
    while radius < n // 2:
        greet(known.at[level], radius)
        pl.semaphore_wait(known.at[level], 2)
        radius, level = 2 * radius, level + 1

    tiles = w_gu.shape[0]
    cols = w_down.shape[0]
    tile = w_gu.shape[2] // 2

    def weight_copies():
        found = []
        for i in range(tiles):
            for j, source in enumerate((gate_hbm, up_hbm)):
                found.append(
                    pltpu.make_async_copy(
                        source.at[0, :, pl.ds(i * tile, tile)],
                        w_gu.at[i, :, pl.ds(j * tile, tile)],
                        w_sem.at[j * tiles + i],
                    )
                )
        for i in range(cols):
            found.append(
                pltpu.make_async_copy(
                    down_hbm.at[0, :, pl.ds(i * SEG, SEG)], w_down.at[i], w_sem.at[2 * tiles + i]
                )
            )
        return found

    for copy in weight_copies():
        copy.start()

    ext[pl.ds(HALO, seq_rows)] = pool_ref[...].astype(F32)
    halo_copy.wait()
    ext[pl.ds(0, HALO)] = jnp.where(me > 0, halo[...].astype(F32), 0.0)
    span = seq_rows + HALO
    levels = []
    reach = 1
    for level in range(lanes):
        kept = ext[pl.ds(0, span)]
        ext[pl.ds(reach, span - reach)] = kept[reach:] + kept[: span - reach]
        levels.append(ext[pl.ds(HALO, seq_rows)])
        reach *= 2
    window_sum = levels[0]
    for level in range(1, lanes):
        window_sum = jnp.where(lane == level, levels[level], window_sum)
    window = jnp.left_shift(jnp.int32(2), lane)
    positions = me * seq_rows + 1 + iota((seq_rows, gdim), 0)
    divisor = jnp.minimum(positions, window).astype(F32)
    pooled = (window_sum / divisor - pool_ref[...].astype(F32)).astype(BF16)
    pieces[...] = (dot(pooled, map_ref[0]) * scale_ref[...].astype(F32)).astype(BF16)

    def piece_copy(k):
        return remote(
            pieces.at[pl.ds(pl.multiple_of(tp_at(k) * tokens, tokens), tokens)],
            piece_in.at[k - 1],
            piece_send.at[k - 1],
            piece_recv.at[k - 1],
            {"tp": tp_at(k)},
        )

    for k in order:
        piece_copy(k).start()
    mix = dot(pieces[pl.ds(pl.multiple_of(lane * tokens, tokens), tokens)], proj_ref[...])
    for k in order:
        proj_copy(k).wait_recv()
        mate_copy(k).start()
    for k in order:
        piece_copy(k).wait_recv()
        settle(proj_in.at[k - 1, other], mate_recv.at[k - 1])
        mix = mix + dot(piece_in[k - 1], proj_in[k - 1])
    mixed_value = (resid_ref[...].astype(F32) + mix).astype(BF16)
    mixed[...] = mixed_value
    residual = mixed_value.astype(F32)
    scaled = residual * lax.rsqrt(
        jnp.sum(residual * residual, axis=1, keepdims=True) / width + norm_eps
    )
    unit = gain_ref.shape[1]
    normed = jnp.concatenate(
        [
            (
                scaled[:, i * unit : (i + 1) * unit] * gain_ref[i : i + 1, :].astype(F32)
            ).astype(BF16)
            for i in range(width // unit)
        ],
        axis=1,
    )
    routed = dot(placing, normed).astype(BF16)
    total[...] = residual

    def to_blocks(value, target):
        for s in range(segs):
            stack[pl.ds(s * crows, crows)] = value[:, s * SEG : (s + 1) * SEG]
        target[...] = dot(spread[...], stack[...]).astype(BF16)

    def send_blocks(source, target, c, send, recv):
        own = pl.ds(pl.multiple_of(me * block, block), block)

        def one(k, carry):
            to = sp_at(k)
            remote(
                source.at[c, pl.ds(pl.multiple_of(to * block, block), block)],
                target.at[c, own],
                send.at[c],
                recv.at[c],
                {"sp": to},
            ).start()
            return carry

        def both(k, carry):
            one(k, 0)
            one(n - k, 0)
            return carry

        lax.fori_loop(1, n // 2, both, 0)
        one(n // 2, 0)

    def take_blocks(source, target, c, recv):
        own = pl.ds(pl.multiple_of(me * block, block), block)
        settle(target.at[c, pl.ds(0, (n - 1) * block)], recv.at[c])
        target[c, own] = source[c, own]
        return dot(gather[...], target[c]).astype(BF16)

    right, left = {"tp": tp_at(1)}, {"tp": tp_at(lanes - 1)}
    low = crows // 2

    def of_lane(k, start, count):
        return pl.ds(pl.multiple_of(tp_at(k) * crows + start, low), count)

    def row_copies(c):
        def one(k, start, i, to):
            at = rows.at[c, of_lane(k, start, low)]
            return remote(at, at, row_send.at[c, i], row_recv.at[c, i], to)

        return (
            one(0, 0, 0, right),
            one(0, low, 1, left),
            one(0, low, 2, right),
            one(0, 0, 3, left),
            one(lanes - 1, 0, 4, right),
            one(1, low, 5, left),
        )

    def part_copies(c):
        def one(k, start, target, i, to):
            at = part.at[c, of_lane(k, start, low)]
            return remote(at, target, part_send.at[c, i], part_recv.at[c, i], to)

        return (
            one(2, 0, far_in.at[c, 0], 0, right),
            one(2, low, far_in.at[c, 1], 1, left),
            one(1, low, part_in.at[c, 0, pl.ds(low, low)], 2, right),
            one(lanes - 1, 0, part_in.at[c, 1, pl.ds(0, low)], 3, left),
            one(1, 0, part_in.at[c, 0, pl.ds(0, low)], 4, right),
            one(lanes - 1, low, part_in.at[c, 1, pl.ds(low, low)], 5, left),
        )

    ahead = min(AHEAD, chunks)
    for c in range(chunks):
        to_blocks(routed[c * crows : (c + 1) * crows], go.at[c])
        if c < ahead:
            send_blocks(go, came, c, go_send, go_recv)
    for copy in weight_copies():
        copy.wait()

    def arrive(c):
        flat = take_blocks(go, came, c, go_recv)
        own = of_lane(0, 0, crows)
        for s in range(segs):
            rows[c, own, s * SEG : (s + 1) * SEG] = flat[s * crows : (s + 1) * crows]
        for copy in row_copies(c)[:4]:
            copy.start()

    def relay(c):
        copies = row_copies(c)
        for i in (0, 1):
            copies[i].wait_recv()
            copies[4 + i].start()

    def experts(c):
        copies = row_copies(c)
        for i in (2, 3, 4, 5):
            copies[i].wait_recv()

        def up_tile(i, carry):
            both = dot(rows[c], w_gu[i])
            g, u = both[:, :tile], both[:, tile:]
            hidden[:, pl.ds(pl.multiple_of(i * tile, tile), tile)] = (
                (g / (1.0 + jnp.exp(-g))) * u
            ).astype(BF16)
            return carry

        lax.fori_loop(0, tiles, up_tile, 0)

        def down_tile(i, carry):
            part[c, :, pl.ds(pl.multiple_of(i * SEG, SEG), SEG)] = dot(
                hidden[...], w_down[i]
            ).astype(BF16)
            return carry

        lax.fori_loop(0, cols, down_tile, 0)
        for copy in part_copies(c)[:4]:
            copy.start()

    def add_far(c):
        copies = part_copies(c)
        for i, (k, start) in enumerate(((1, 0), (lanes - 1, low))):
            copies[i].wait_recv()
            at = of_lane(k, start, low)
            part[c, at] = (part[c, at].astype(F32) + far_in[c, i].astype(F32)).astype(BF16)
            copies[4 + i].start()

    def give_back(c):
        copies = part_copies(c)
        for i in (2, 3, 4, 5):
            copies[i].wait_recv()
        value = part[c, of_lane(0, 0, crows)].astype(F32)
        value = value + part_in[c, 0].astype(F32) + part_in[c, 1].astype(F32)
        to_blocks(value.astype(BF16), back.at[c])
        send_blocks(back, home, c, back_send, back_recv)

    def combine(c):
        flat = take_blocks(back, home, c, back_recv)
        sides = (((0,), (0,)), ((), ()))
        for s in range(segs):
            piece = flat[s * crows : (s + 1) * crows]
            cut = pl.ds(s * SEG, SEG)
            total[:, cut] += lax.dot_general(
                w_hi[c], piece, sides, preferred_element_type=F32
            ) + lax.dot_general(w_lo[c], piece, sides, preferred_element_type=F32)

    def send_next(c):
        send_blocks(go, came, c, go_send, go_recv)

    stages = {
        "arrive": arrive,
        "relay": relay,
        "experts": experts,
        "add_far": add_far,
        "give_back": give_back,
        "combine": combine,
        "send_next": send_next,
    }

    def step(k, carry):
        for name, lag in SCHEDULE:
            c = k - lag
            low_end = ahead if name == "send_next" else 0

            @pl.when((c >= low_end) & (c < chunks))
            def _():
                stages[name](c)

        return carry

    lax.fori_loop(0, chunks + max(lag for _, lag in SCHEDULE), step, 0)
    out_ref[...] = total[...].astype(BF16)

    for k in order:
        proj_copy(k).wait_send()
        mate_copy(k).wait_send()
        piece_copy(k).wait_send()

    def drain(c, carry):
        settle(go.at[c, pl.ds(0, (n - 1) * block)], go_send.at[c])
        settle(back.at[c, pl.ds(0, (n - 1) * block)], back_send.at[c])
        for copy in row_copies(c) + part_copies(c):
            copy.wait_send()
        return carry

    lax.fori_loop(0, chunks, drain, 0)


def local(
    resid,
    pool_input,
    group_map,
    pool_scale,
    out_proj,
    norm_gain,
    routes,
    route_weight,
    expert_gate,
    expert_up,
    expert_down,
):
    n, lanes = lax.axis_size("sp"), lax.axis_size("tp")
    tokens, width = resid.shape
    seq_rows, gdim = pool_input.shape
    ff = expert_gate.shape[2]
    slots = max(2, 5 * tokens * routes.shape[1] // (4 * n))
    chunks = slots // PAIR
    assert chunks * PAIR == slots and lanes == 4
    segs = width // SEG
    size = n * PAIR * segs
    crows = PAIR * n
    tile = min(128, ff)
    tiles, cols = ff // tile, width // SEG
    vmem, dma = pltpu.VMEM, pltpu.SemaphoreType.DMA
    hbm = pl.BlockSpec(memory_space=pl.ANY)
    scratch = [
        vmem((HALO + seq_rows, gdim), F32),
        vmem((HALO, gdim), BF16),
        vmem((seq_rows, gdim), BF16),
        vmem((lanes - 1, tokens, gdim), BF16),
        vmem((lanes - 1, gdim, width), BF16),
        vmem((tokens, width), BF16),
        vmem((size, size), BF16),
        vmem((size, size), BF16),
        vmem((chunks, crows, tokens), BF16),
        vmem((chunks, crows, tokens), BF16),
        vmem((tiles, width, 2 * tile), BF16),
        vmem((cols, ff, SEG), BF16),
        vmem((size, SEG), BF16),
        vmem((chunks, size, SEG), BF16),
        vmem((chunks, size, SEG), BF16),
        vmem((chunks, lanes * crows, width), BF16),
        vmem((lanes * crows, ff), BF16),
        vmem((chunks, lanes * crows, width), BF16),
        vmem((chunks, 2, crows, width), BF16),
        vmem((chunks, 2, crows // 2, width), BF16),
        vmem((chunks, size, SEG), BF16),
        vmem((chunks, size, SEG), BF16),
        vmem((tokens, width), F32),
        pltpu.SemaphoreType.REGULAR((max(1, n.bit_length()),)),
        dma((2 * tiles + cols,)),
        dma((2,)),
        dma((lanes - 1,)),
        dma((lanes - 1,)),
        dma((lanes - 1,)),
        dma((lanes - 1,)),
        dma((lanes - 1,)),
        dma((lanes - 1,)),
        dma((chunks,)),
        dma((chunks,)),
        dma((chunks, 6)),
        dma((chunks, 6)),
        dma((chunks, 6)),
        dma((chunks, 6)),
        dma((chunks,)),
        dma((chunks,)),
    ]
    return pl.pallas_call(
        functools.partial(kernel, (n, lanes, chunks, slots)),
        out_shape=jax.ShapeDtypeStruct((tokens, width), BF16),
        in_specs=[pl.BlockSpec(memory_space=vmem)] * 8 + [hbm] * 3,
        out_specs=pl.BlockSpec(memory_space=vmem),
        scratch_shapes=scratch,
        compiler_params=pltpu.CompilerParams(
            collective_id=0, has_side_effects=True, vmem_limit_bytes=60 * 1024 * 1024
        ),
        name="layer",
    )(
        resid,
        pool_input,
        group_map,
        pool_scale.reshape(1, -1),
        out_proj,
        norm_gain.reshape(-1, 128),
        routes.T,
        route_weight.T,
        expert_gate,
        expert_up,
        expert_down,
    )


def solution(mesh):
    return jax.shard_map(
        local,
        mesh=mesh,
        in_specs=(
            P(("grp", "sp", "tp"), None),
            P(("grp", "sp"), "tp"),
            P("tp", None, None),
            P("tp"),
            P("tp", None),
            P(),
            P(("grp", "sp", "tp"), None),
            P(("grp", "sp", "tp"), None),
            P("sp", None, "tp"),
            P("sp", None, "tp"),
            P("sp", "tp", None),
        ),
        out_specs=P(("grp", "sp", "tp"), None),
        check_vma=False,
    )
```

```python
import functools

import jax
import jax.numpy as jnp
from jax import lax
from jax.experimental import pallas as pl
from jax.experimental.pallas import tpu as pltpu
from jax.sharding import PartitionSpec as P

MESH = pl.DeviceIdType.MESH
BF16 = jnp.bfloat16
F32 = jnp.float32
I32 = jnp.int32

norm_eps = 1e-06
PAIR = 2
SEG = 256
HALO = 16
AHEAD = 2

SCHEDULE = (
    ("arrive", 0),
    ("send_next", -AHEAD),
    ("experts", 1),
    ("relay", 0),
    ("give_back", 2),
    ("add_far", 1),
    ("combine", 4),
)


def iota(shape, dim):
    return lax.broadcasted_iota(I32, shape, dim)


def dot(a, b):
    return jnp.dot(a, b, preferred_element_type=F32)


def quot(a, b):
    return jnp.right_shift(a, b.bit_length() - 1) if b & (b - 1) == 0 else a // b


def rem(a, b):
    return jnp.bitwise_and(a, b - 1) if b & (b - 1) == 0 else lax.rem(a, b)


def settle(like, sem):
    pltpu.make_async_copy(like, like, sem).wait()


def kernel(
    sizes,
    resid_hbm,
    pool_hbm,
    map_hbm,
    scale_hbm,
    proj_hbm,
    gain_hbm,
    routes_hbm,
    weight_hbm,
    gate_hbm,
    up_hbm,
    down_hbm,
    out_ref,
    pool_ref,
    map_ref,
    scale_ref,
    proj_ref,
    gain_ref,
    routes_ref,
    weight_ref,
    ext,
    halo,
    pieces,
    piece_in,
    proj_in,
    mixed,
    spread,
    gather,
    w_hi,
    w_lo,
    w_gu,
    w_down,
    stack,
    go,
    came,
    rows,
    hidden,
    part,
    part_in,
    far_in,
    back,
    home,
    total,
    known,
    resid_sem,
    in_sem,
    w_sem,
    halo_sem,
    proj_send,
    proj_recv,
    mate_send,
    mate_recv,
    piece_send,
    piece_recv,
    go_send,
    go_recv,
    row_send,
    row_recv,
    part_send,
    part_recv,
    back_send,
    back_recv,
):
    n, lanes, chunks, slots = sizes
    tokens, width = resid_hbm.shape
    seq_rows, gdim = pool_hbm.shape
    segs = width // SEG
    block = PAIR * segs
    crows = PAIR * n
    half = gdim // 2
    me = lax.axis_index("sp")
    lane = lax.axis_index("tp")
    core = lax.rem(me, 2)
    mate = me + 1 - 2 * core

    def sp_at(k):
        return lax.rem(me + k, n)

    def tp_at(k):
        return lax.rem(lane + k, lanes)

    def remote(src, dst, send, recv, where):
        return pltpu.make_async_remote_copy(
            src_ref=src,
            dst_ref=dst,
            send_sem=send,
            recv_sem=recv,
            device_id=where,
            device_id_type=MESH,
        )

    barrier = pltpu.get_barrier_semaphore()

    def greet(sem, radius):
        for k in (radius, n - radius):
            pl.semaphore_signal(
                sem, inc=1, device_id={"sp": sp_at(k)}, device_id_type=MESH
            )

    greet(barrier, 1)
    for k in range(1, lanes):
        pl.semaphore_signal(
            barrier, inc=1, device_id={"tp": tp_at(k)}, device_id_type=MESH
        )

    small = {
        name: pltpu.make_async_copy(source, target, in_sem.at[i])
        for i, (name, source, target) in enumerate(
            (
                ("proj", proj_hbm, proj_ref),
                ("pool", pool_hbm, pool_ref),
                ("map", map_hbm, map_ref),
                ("scale", scale_hbm, scale_ref),
                ("gain", gain_hbm, gain_ref),
                ("routes", routes_hbm, routes_ref),
                ("weight", weight_hbm, weight_ref),
            )
        )
    }
    for copy in small.values():
        copy.start()
    small["pool"].wait()
    small["proj"].wait()
    pl.semaphore_wait(barrier, 2 + lanes - 1)

    halo_copy = remote(
        pool_ref.at[pl.ds(seq_rows - HALO, HALO)],
        halo,
        halo_sem.at[0],
        halo_sem.at[1],
        {"sp": sp_at(1)},
    )
    halo_copy.start()
    mine = pl.ds(pl.multiple_of(core * half, half), half)
    other = pl.ds(pl.multiple_of((1 - core) * half, half), half)

    def proj_copy(k):
        return remote(
            proj_ref.at[mine],
            proj_in.at[k - 1, mine],
            proj_send.at[k - 1],
            proj_recv.at[k - 1],
            {"tp": tp_at(k)},
        )

    def mate_copy(k):
        return remote(
            proj_in.at[k - 1, mine],
            proj_in.at[k - 1, mine],
            mate_send.at[k - 1],
            mate_recv.at[k - 1],
            {"sp": mate},
        )

    order = [k for k in (1, 3, 2) if k < lanes]
    for k in order:
        proj_copy(k).start()

    size = n * block

    def block_row(a):
        rest = rem(a, crows)
        return quot(rest, PAIR) * block + quot(a, crows) * PAIR + rem(rest, PAIR)

    def fill_gather():
        gather[...] = jnp.where(
            iota((size, size), 1) == block_row(iota((size, 1), 0)), 1.0, 0.0
        ).astype(BF16)

    def fill_spread():
        spread[...] = jnp.where(
            iota((size, size), 0) == block_row(iota((1, size), 1)), 1.0, 0.0
        ).astype(BF16)

    resid_copy = pltpu.make_async_copy(resid_hbm, mixed, resid_sem)
    resid_copy.start()

    radius, level = 1, 0
    work = [fill_gather, fill_spread]
    while radius < n // 2:
        greet(known.at[level], radius)
        if work:
            work.pop(0)()
        pl.semaphore_wait(known.at[level], 2)
        radius, level = 2 * radius, level + 1
    for left_over in work:
        left_over()

    for name in ("map", "scale", "gain", "routes", "weight"):
        small[name].wait()
    one0 = (iota((n, tokens), 0) == routes_ref[0:1, :]).astype(F32)
    one1 = (iota((n, tokens), 0) == routes_ref[1:2, :]).astype(F32)
    before = (iota((tokens, tokens), 0) < iota((tokens, tokens), 1)).astype(F32).astype(BF16)
    rank0 = dot(one0.astype(BF16), before)
    rank1 = dot(one1.astype(BF16), before) + jnp.sum(one0, axis=1, keepdims=True)
    slot0 = jnp.sum(rank0 * one0, axis=0, keepdims=True).astype(I32)
    slot1 = jnp.sum(rank1 * one1, axis=0, keepdims=True).astype(I32)
    row0 = quot(slot0, PAIR) * crows + routes_ref[0:1, :] * PAIR + rem(slot0, PAIR)
    row1 = quot(slot1, PAIR) * crows + routes_ref[1:2, :] * PAIR + rem(slot1, PAIR)
    place = iota((chunks * crows, tokens), 0)
    hit0, hit1 = place == row0, place == row1
    weight = jnp.where(hit0, weight_ref[0:1, :], 0.0) + jnp.where(hit1, weight_ref[1:2, :], 0.0)
    high = weight.astype(BF16)
    w_hi[...] = high.reshape(chunks, crows, tokens)
    w_lo[...] = (weight - high.astype(F32)).astype(BF16).reshape(chunks, crows, tokens)
    placing = (jnp.where(hit0, 1.0, 0.0) + jnp.where(hit1, 1.0, 0.0)).astype(BF16)

    tiles = w_gu.shape[0]
    cols = w_down.shape[0]
    tile = w_gu.shape[2] // 2

    def weight_copies():
        found = []
        for i in range(tiles):
            for j, source in enumerate((gate_hbm, up_hbm)):
                found.append(
                    pltpu.make_async_copy(
                        source.at[0, :, pl.ds(i * tile, tile)],
                        w_gu.at[i, :, pl.ds(j * tile, tile)],
                        w_sem.at[j * tiles + i],
                    )
                )
        for i in range(cols):
            found.append(
                pltpu.make_async_copy(
                    down_hbm.at[0, :, pl.ds(i * SEG, SEG)], w_down.at[i], w_sem.at[2 * tiles + i]
                )
            )
        return found

    for copy in weight_copies():
        copy.start()

    ext[pl.ds(HALO, seq_rows)] = pool_ref[...].astype(F32)
    halo_copy.wait()
    ext[pl.ds(0, HALO)] = jnp.where(me > 0, halo[...].astype(F32), 0.0)
    span = seq_rows + HALO
    levels = []
    reach = 1
    for level in range(lanes):
        kept = ext[pl.ds(0, span)]
        ext[pl.ds(reach, span - reach)] = kept[reach:] + kept[: span - reach]
        levels.append(ext[pl.ds(HALO, seq_rows)])
        reach *= 2
    window_sum = levels[0]
    for level in range(1, lanes):
        window_sum = jnp.where(lane == level, levels[level], window_sum)
    window = jnp.left_shift(jnp.int32(2), lane)
    positions = me * seq_rows + 1 + iota((seq_rows, gdim), 0)
    divisor = jnp.minimum(positions, window).astype(F32)
    pooled = (window_sum / divisor - pool_ref[...].astype(F32)).astype(BF16)
    pieces[...] = (dot(pooled, map_ref[0]) * scale_ref[...].astype(F32)).astype(BF16)

    def piece_copy(k):
        return remote(
            pieces.at[pl.ds(pl.multiple_of(tp_at(k) * tokens, tokens), tokens)],
            piece_in.at[k - 1],
            piece_send.at[k - 1],
            piece_recv.at[k - 1],
            {"tp": tp_at(k)},
        )

    for k in order:
        piece_copy(k).start()
    mix = dot(pieces[pl.ds(pl.multiple_of(lane * tokens, tokens), tokens)], proj_ref[...])
    for k in order:
        proj_copy(k).wait_recv()
        mate_copy(k).start()
    for k in order:
        piece_copy(k).wait_recv()
        settle(proj_in.at[k - 1, other], mate_recv.at[k - 1])
        mix = mix + dot(piece_in[k - 1], proj_in[k - 1])
    resid_copy.wait()
    mixed_value = (mixed[...].astype(F32) + mix).astype(BF16)
    residual = mixed_value.astype(F32)
    scaled = residual * lax.rsqrt(
        jnp.sum(residual * residual, axis=1, keepdims=True) / width + norm_eps
    )
    unit = gain_ref.shape[1]
    normed = jnp.concatenate(
        [
            (
                scaled[:, i * unit : (i + 1) * unit] * gain_ref[i : i + 1, :].astype(F32)
            ).astype(BF16)
            for i in range(width // unit)
        ],
        axis=1,
    )
    routed = dot(placing, normed).astype(BF16)
    total[...] = residual

    def to_blocks(value, target):
        for s in range(segs):
            stack[pl.ds(s * crows, crows)] = value[:, s * SEG : (s + 1) * SEG]
        target[...] = dot(spread[...], stack[...]).astype(BF16)

    def send_blocks(source, target, c, send, recv):
        own = pl.ds(pl.multiple_of(me * block, block), block)

        def one(k, carry):
            to = sp_at(k)
            remote(
                source.at[c, pl.ds(pl.multiple_of(to * block, block), block)],
                target.at[c, own],
                send.at[c],
                recv.at[c],
                {"sp": to},
            ).start()
            return carry

        def both(k, carry):
            one(n // 2 - k, 0)
            one(n // 2 + k, 0)
            return carry

        one(n // 2, 0)
        lax.fori_loop(1, n // 2, both, 0)

    def take_blocks(source, target, c, recv):
        own = pl.ds(pl.multiple_of(me * block, block), block)
        settle(target.at[c, pl.ds(0, (n - 1) * block)], recv.at[c])
        target[c, own] = source[c, own]
        return dot(gather[...], target[c]).astype(BF16)

    right, left = {"tp": tp_at(1)}, {"tp": tp_at(lanes - 1)}
    low = crows // 2

    def of_lane(k, start, count):
        return pl.ds(pl.multiple_of(tp_at(k) * crows + start, low), count)

    def row_copies(c):
        def one(k, start, i, to):
            at = rows.at[c, of_lane(k, start, low)]
            return remote(at, at, row_send.at[c, i], row_recv.at[c, i], to)

        return (
            one(0, 0, 0, right),
            one(0, low, 1, left),
            one(0, low, 2, right),
            one(0, 0, 3, left),
            one(lanes - 1, 0, 4, right),
            one(1, low, 5, left),
        )

    def part_copies(c):
        def one(k, start, target, i, to):
            at = part.at[c, of_lane(k, start, low)]
            return remote(at, target, part_send.at[c, i], part_recv.at[c, i], to)

        return (
            one(2, 0, far_in.at[c, 0], 0, right),
            one(2, low, far_in.at[c, 1], 1, left),
            one(1, low, part_in.at[c, 0, pl.ds(low, low)], 2, right),
            one(lanes - 1, 0, part_in.at[c, 1, pl.ds(0, low)], 3, left),
            one(1, 0, part_in.at[c, 0, pl.ds(0, low)], 4, right),
            one(lanes - 1, low, part_in.at[c, 1, pl.ds(low, low)], 5, left),
        )

    ahead = min(AHEAD, chunks)
    for c in range(chunks):
        to_blocks(routed[c * crows : (c + 1) * crows], go.at[c])
        if c < ahead:
            send_blocks(go, came, c, go_send, go_recv)
    for copy in weight_copies():
        copy.wait()

    def arrive(c):
        flat = take_blocks(go, came, c, go_recv)
        own = of_lane(0, 0, crows)
        for s in range(segs):
            rows[c, own, s * SEG : (s + 1) * SEG] = flat[s * crows : (s + 1) * crows]
        for copy in row_copies(c)[:4]:
            copy.start()

    def relay(c):
        copies = row_copies(c)
        for i in (0, 1):
            copies[i].wait_recv()
            copies[4 + i].start()

    def experts(c):
        copies = row_copies(c)
        for i in (2, 3, 4, 5):
            copies[i].wait_recv()

        def up_tile(i, carry):
            both = dot(rows[c], w_gu[i])
            g, u = both[:, :tile], both[:, tile:]
            hidden[:, pl.ds(pl.multiple_of(i * tile, tile), tile)] = (
                (g / (1.0 + jnp.exp(-g))) * u
            ).astype(BF16)
            return carry

        lax.fori_loop(0, tiles, up_tile, 0)

        def down_tile(i, carry):
            part[c, :, pl.ds(pl.multiple_of(i * SEG, SEG), SEG)] = dot(
                hidden[...], w_down[i]
            ).astype(BF16)
            return carry

        lax.fori_loop(0, cols, down_tile, 0)
        for copy in part_copies(c)[:4]:
            copy.start()

    def add_far(c):
        copies = part_copies(c)
        for i, (k, start) in enumerate(((1, 0), (lanes - 1, low))):
            copies[i].wait_recv()
            at = of_lane(k, start, low)
            part[c, at] = (part[c, at].astype(F32) + far_in[c, i].astype(F32)).astype(BF16)
            copies[4 + i].start()

    def give_back(c):
        copies = part_copies(c)
        for i in (2, 3, 4, 5):
            copies[i].wait_recv()
        value = part[c, of_lane(0, 0, crows)].astype(F32)
        value = value + part_in[c, 0].astype(F32) + part_in[c, 1].astype(F32)
        to_blocks(value.astype(BF16), back.at[c])
        send_blocks(back, home, c, back_send, back_recv)

    def combine(c):
        flat = take_blocks(back, home, c, back_recv)
        sides = (((0,), (0,)), ((), ()))
        for s in range(segs):
            piece = flat[s * crows : (s + 1) * crows]
            cut = pl.ds(s * SEG, SEG)
            total[:, cut] += lax.dot_general(
                w_hi[c], piece, sides, preferred_element_type=F32
            ) + lax.dot_general(w_lo[c], piece, sides, preferred_element_type=F32)

    def send_next(c):
        send_blocks(go, came, c, go_send, go_recv)

    stages = {
        "arrive": arrive,
        "relay": relay,
        "experts": experts,
        "add_far": add_far,
        "give_back": give_back,
        "combine": combine,
        "send_next": send_next,
    }

    def step(k, carry):
        for name, lag in SCHEDULE:
            c = k - lag
            low_end = ahead if name == "send_next" else 0

            @pl.when((c >= low_end) & (c < chunks))
            def _():
                stages[name](c)

        return carry

    lax.fori_loop(0, chunks + max(lag for _, lag in SCHEDULE), step, 0)
    out_ref[...] = total[...].astype(BF16)

    for k in order:
        proj_copy(k).wait_send()
        mate_copy(k).wait_send()
        piece_copy(k).wait_send()

    def drain(c, carry):
        settle(go.at[c, pl.ds(0, (n - 1) * block)], go_send.at[c])
        settle(back.at[c, pl.ds(0, (n - 1) * block)], back_send.at[c])
        for copy in row_copies(c) + part_copies(c):
            copy.wait_send()
        return carry

    lax.fori_loop(0, chunks, drain, 0)


def local(
    resid,
    pool_input,
    group_map,
    pool_scale,
    out_proj,
    norm_gain,
    routes,
    route_weight,
    expert_gate,
    expert_up,
    expert_down,
):
    n, lanes = lax.axis_size("sp"), lax.axis_size("tp")
    tokens, width = resid.shape
    seq_rows, gdim = pool_input.shape
    ff = expert_gate.shape[2]
    slots = max(2, 5 * tokens * routes.shape[1] // (4 * n))
    chunks = slots // PAIR
    assert chunks * PAIR == slots and lanes == 4
    segs = width // SEG
    size = n * PAIR * segs
    crows = PAIR * n
    tile = min(128, ff)
    tiles, cols = ff // tile, width // SEG
    vmem, dma = pltpu.VMEM, pltpu.SemaphoreType.DMA
    hbm = pl.BlockSpec(memory_space=pl.ANY)
    scratch = [
        vmem(pool_input.shape, BF16),
        vmem(group_map.shape, BF16),
        vmem((1, gdim), BF16),
        vmem(out_proj.shape, BF16),
        vmem((width // 128, 128), BF16),
        vmem(routes.shape[::-1], I32),
        vmem(route_weight.shape[::-1], F32),
        vmem((HALO + seq_rows, gdim), F32),
        vmem((HALO, gdim), BF16),
        vmem((seq_rows, gdim), BF16),
        vmem((lanes - 1, tokens, gdim), BF16),
        vmem((lanes - 1, gdim, width), BF16),
        vmem((tokens, width), BF16),
        vmem((size, size), BF16),
        vmem((size, size), BF16),
        vmem((chunks, crows, tokens), BF16),
        vmem((chunks, crows, tokens), BF16),
        vmem((tiles, width, 2 * tile), BF16),
        vmem((cols, ff, SEG), BF16),
        vmem((size, SEG), BF16),
        vmem((chunks, size, SEG), BF16),
        vmem((chunks, size, SEG), BF16),
        vmem((chunks, lanes * crows, width), BF16),
        vmem((lanes * crows, ff), BF16),
        vmem((chunks, lanes * crows, width), BF16),
        vmem((chunks, 2, crows, width), BF16),
        vmem((chunks, 2, crows // 2, width), BF16),
        vmem((chunks, size, SEG), BF16),
        vmem((chunks, size, SEG), BF16),
        vmem((tokens, width), F32),
        pltpu.SemaphoreType.REGULAR((max(1, n.bit_length()),)),
        dma,
        dma((7,)),
        dma((2 * tiles + cols,)),
        dma((2,)),
        dma((lanes - 1,)),
        dma((lanes - 1,)),
        dma((lanes - 1,)),
        dma((lanes - 1,)),
        dma((lanes - 1,)),
        dma((lanes - 1,)),
        dma((chunks,)),
        dma((chunks,)),
        dma((chunks, 6)),
        dma((chunks, 6)),
        dma((chunks, 6)),
        dma((chunks, 6)),
        dma((chunks,)),
        dma((chunks,)),
    ]
    return pl.pallas_call(
        functools.partial(kernel, (n, lanes, chunks, slots)),
        out_shape=jax.ShapeDtypeStruct((tokens, width), BF16),
        in_specs=[hbm] * 11,
        out_specs=pl.BlockSpec(memory_space=vmem),
        scratch_shapes=scratch,
        compiler_params=pltpu.CompilerParams(
            collective_id=0, has_side_effects=True, vmem_limit_bytes=60 * 1024 * 1024
        ),
        name="layer",
    )(
        resid,
        pool_input,
        group_map,
        pool_scale.reshape(1, -1),
        out_proj,
        norm_gain.reshape(-1, 128),
        routes.T,
        route_weight.T,
        expert_gate,
        expert_up,
        expert_down,
    )


def solution(mesh):
    return jax.shard_map(
        local,
        mesh=mesh,
        in_specs=(
            P(("grp", "sp", "tp"), None),
            P(("grp", "sp"), "tp"),
            P("tp", None, None),
            P("tp"),
            P("tp", None),
            P(),
            P(("grp", "sp", "tp"), None),
            P(("grp", "sp", "tp"), None),
            P("sp", None, "tp"),
            P("sp", None, "tp"),
            P("sp", "tp", None),
        ),
        out_specs=P(("grp", "sp", "tp"), None),
        check_vma=False,
    )
```
